32 devices in a mesh: sp: 8 (over z, x), tp: 4 (over y, core).
Axes of the slice: x: 2, y: 2, z: 4, core: 2. Of those that a mesh axis runs over, the one named last changes fastest.
Arguments:
- layer_input: bfloat16 [8, 1536, 2048], P('sp', 'tp'), may hold values from -6 to 6
- input_gain: float32 [2048], replicated, may hold values from 0.1 to 1.9
- key_weight: bfloat16 [2048, 512], P('sp', 'tp'), may hold values from -0.125 to 0.125
- value_weight: bfloat16 [2048, 512], P('sp', 'tp'), may hold values from -0.125 to 0.125
- key_gain: float32 [128], replicated, may hold values from 0.1 to 1.9
- stop_shift: bfloat16 [8, 4, 1536], P('sp', None, 'tp'), may hold values from -20 to 0
- new_query: bfloat16 [8, 16, 128], P('sp', 'tp'), may hold values from -6 to 6
- query_gain: float32 [128], replicated, may hold values from 0.1 to 1.9
- out_gain: float32 [128], replicated, may hold values from 0.1 to 1.9
Outputs:
- key_cache: bfloat16 [8, 4, 1536, 128], P('sp', 'tp')
- value_cache: bfloat16 [8, 4, 1536, 128], P('sp', 'tp')
- shift_cache: bfloat16 [8, 4, 1536], P('sp', 'tp')
- first_read: bfloat16 [8, 16, 128], P('sp', 'tp')
The draws below stay inside these ranges and needn't reach their ends.
All inputs are finite; a program needn't handle non-finite values.
Results may differ from the reference program's by a relative error of at most 0.013.
Values may be sent and summed in bfloat16 or wider, within the bound.
A program may use at most 64 MiB of HBM per device.

```python
import math
import jax
import jax.numpy as jnp
from jax import lax

D = 2048
HQ = 16
KVH = 4
HEAD = 128
TOK_DEV = 384
PROMPT_LENGTH = 1536
SEQS = 8
COPIES = 1


def draw_stop_shift(key, part):
    order_key, slow_key, fast_key, block_key, cell_key, place_key, level_key = jax.random.split(key, 7)
    head_order = jax.random.permutation(order_key, KVH)
    slow_heads = (head_order < KVH // 2)[None, :, None]
    slow_rate = jax.random.uniform(slow_key, (SEQS, KVH, 1), jnp.float32, math.log(0.1 / PROMPT_LENGTH), math.log(1.0 / PROMPT_LENGTH))
    fast_rate = jax.random.uniform(fast_key, (SEQS, KVH, 1), jnp.float32, math.log(4.0 / TOK_DEV), math.log(12.0 / TOK_DEV))
    log_rate = jnp.where(slow_heads, slow_rate, fast_rate)
    blocks = jax.random.uniform(block_key, (SEQS, KVH, PROMPT_LENGTH // TOK_DEV, 1), jnp.float32, -0.7, 0.7)
    blocks = jnp.broadcast_to(blocks, (SEQS, KVH, PROMPT_LENGTH // TOK_DEV, TOK_DEV)).reshape(SEQS, KVH, PROMPT_LENGTH)
    cell_noise = jax.random.uniform(cell_key, (SEQS, KVH, PROMPT_LENGTH), jnp.float32, -0.7, 0.7)
    baseline_offset = jnp.minimum(log_rate + blocks + cell_noise, -0.5)
    token_positions = jax.random.randint(place_key, (SEQS, 1, 1, 4), 0, PROMPT_LENGTH)
    spike_mask = jnp.any(jnp.arange(PROMPT_LENGTH)[None, None, :, None] == token_positions, axis=-1)
    depth_levels = jax.random.uniform(level_key, (SEQS, KVH, PROMPT_LENGTH), jnp.float32, -1.4, 0.0)
    return jnp.where(spike_mask, depth_levels, baseline_offset).astype(jnp.bfloat16)


def levels(rng, dims, cuts, low, top_value):
    def one(axis_at, blocks):
        draws = jax.random.uniform(jax.random.fold_in(jax.random.fold_in(rng, 6), axis_at), (blocks,), jnp.float32, low / len(cuts), top_value / len(cuts))
        return jnp.repeat(jnp.exp(draws), dims[axis_at] // blocks).reshape((-1,) + (1,) * (len(dims) - axis_at - 1))

    level = one(*cuts[0])
    for cut in cuts[1:]:
        level = level * one(*cut)
    return level


def normal_values(rng, shape, spread, limit, cuts=(), dtype=jnp.bfloat16):
    entries = jax.random.normal(rng, shape, jnp.float32) * spread
    if len(cuts) > 0:
        entries = levels(rng, shape, cuts, -0.22, 0.18) * entries
    return jnp.clip(entries, min=-limit, max=limit).astype(dtype)


def setup_inputs(seed: int = 0) -> dict:
    key_of = jax.random.split(jax.random.key(seed), 10)
    layer_input = normal_values(key_of[0], (SEQS, PROMPT_LENGTH, D), 1.0, 6.0, ((0, 8), (1, 4)))
    input_gain = jnp.clip(1.0 + 0.18 * jax.random.normal(key_of[1], (D,), jnp.float32), 0.1, 1.9)
    key_weight = normal_values(key_of[2], (D, KVH * HEAD), D ** -0.5, 0.125, ((0, 8), (1, 4)))
    value_weight = normal_values(key_of[3], (D, KVH * HEAD), D ** -0.5, 0.125, ((0, 8), (1, 4)))
    key_gain = jnp.clip(1.0 + 0.18 * jax.random.normal(key_of[4], (HEAD,), jnp.float32), 0.1, 1.9)
    stop_shift = draw_stop_shift(jax.random.fold_in(key_of[9], 71), 0)
    new_query = normal_values(key_of[6], (SEQS, HQ, HEAD), 1.0, 6.0, ((0, 8), (1, 4)))
    query_gain = jnp.clip(1.0 + 0.18 * jax.random.normal(key_of[7], (HEAD,), jnp.float32), 0.1, 1.9)
    out_gain = jnp.clip(1.0 + 0.18 * jax.random.normal(key_of[8], (HEAD,), jnp.float32), 0.1, 1.9)
    return dict(layer_input=layer_input, input_gain=input_gain, key_weight=key_weight, value_weight=value_weight, key_gain=key_gain, stop_shift=stop_shift, new_query=new_query, query_gain=query_gain, out_gain=out_gain)


epsilon = 1e-06

def row_norm(value_entries, scaling):
    return value_entries * lax.rsqrt(lax.optimization_barrier(jnp.mean(value_entries * value_entries, axis=-1, keepdims=True)) + epsilon) * scaling

def reference(layer_input, input_gain, key_weight, value_weight, key_gain, stop_shift, new_query, query_gain, out_gain):
    group_size = HQ // KVH
    score_scale = 1.0 / HEAD ** 0.5

    def one_sequence(sequence):
        tokens, shifts, queries = sequence
        normed = row_norm(tokens.astype(jnp.float32), input_gain).astype(jnp.bfloat16)
        raw_keys = jnp.dot(normed, key_weight, preferred_element_type=jnp.float32).reshape(PROMPT_LENGTH, KVH, HEAD)
        key_rows = row_norm(raw_keys, key_gain).astype(jnp.bfloat16)
        value_rows = jnp.dot(normed, value_weight, preferred_element_type=jnp.float32).astype(jnp.bfloat16).reshape(PROMPT_LENGTH, KVH, HEAD)
        query_rows = row_norm(queries.astype(jnp.float32), query_gain).astype(jnp.bfloat16).reshape(KVH, group_size, HEAD)
        scores = jnp.einsum('kgd,lkd->kgl', query_rows.astype(jnp.float32), key_rows.astype(jnp.float32)) * score_scale
        scores = scores + shifts.astype(jnp.float32)[:, None, :]
        log_keep = jax.nn.log_sigmoid(-scores)
        later_sum = lax.cumsum(log_keep, axis=2, reverse=True) - log_keep
        weights = jnp.exp(jax.nn.log_sigmoid(scores) + later_sum).astype(jnp.bfloat16)
        read_sum = jnp.einsum('kgl,lkd->kgd', weights.astype(jnp.float32), value_rows.astype(jnp.float32)).reshape(HQ, HEAD)
        first_out = row_norm(read_sum, out_gain).astype(jnp.bfloat16)
        key_slots = jnp.repeat(key_rows.transpose(1, 0, 2), COPIES, axis=0)
        value_slots = jnp.repeat(value_rows.transpose(1, 0, 2), COPIES, axis=0)
        shift_slots = jnp.repeat(shifts, COPIES, axis=0)
        return (key_slots, value_slots, shift_slots, first_out)
    key_cache, value_cache, shift_cache, first_read = lax.map(one_sequence, (layer_input, stop_shift, new_query))
    return (key_cache, value_cache, shift_cache, first_read)
```

```python
import functools

import jax
import jax.numpy as jnp
from jax import lax
from jax.experimental import pallas as pl
from jax.experimental.pallas import tpu as pltpu
from jax.sharding import PartitionSpec as P

KVH = 4


epsilon = 1e-06


def row_norm(value_entries, scaling):
    return (
        value_entries
        * lax.rsqrt(jnp.mean(value_entries * value_entries, axis=-1, keepdims=True) + epsilon)
        * scaling
    )


def shards(
    layer_input,
    input_gain,
    key_weight,
    value_weight,
    key_gain,
    stop_shift,
    new_query,
    query_gain,
    out_gain,
):
    groups = lax.axis_size("tp")
    copies = groups // KVH
    row_count = layer_input.shape[1]
    head_size = new_query.shape[2]
    score_scale = 1.0 / head_size**0.5
    normed = row_norm(layer_input[0].astype(jnp.float32), input_gain).astype(jnp.bfloat16)
    stacked = jnp.stack((key_weight, value_weight), 0)
    full_depth = lax.all_gather(stacked, "sp", axis=1, tiled=True)
    projected = jnp.einsum(
        "rd,kdc->krc",
        normed,
        lax.all_gather(full_depth, "tp", axis=2, tiled=True),
        preferred_element_type=jnp.float32,
    )
    key_rows = row_norm(projected[0].reshape(row_count, KVH, head_size), key_gain).astype(
        jnp.bfloat16
    )
    value_rows = projected[1].reshape(row_count, KVH, head_size).astype(jnp.bfloat16)
    local_shift = stop_shift[0]
    key_slots = jnp.repeat(key_rows, copies, axis=1)
    value_slots = jnp.repeat(value_rows, copies, axis=1)
    shift_slots = jnp.repeat(local_shift.T, copies, axis=1)
    key_got, value_got, shift_got = (
        lax.all_to_all(key_slots, "tp", split_axis=1, concat_axis=0, tiled=True),
        lax.all_to_all(value_slots, "tp", split_axis=1, concat_axis=0, tiled=True),
        lax.all_to_all(shift_slots, "tp", split_axis=1, concat_axis=0, tiled=True),
    )
    key_line = key_got[:, 0, :]
    value_line = value_got[:, 0, :]
    shift_line = shift_got[:, 0]
    length = key_line.shape[0]
    query_rows = row_norm(new_query[0].astype(jnp.float32), query_gain).astype(jnp.bfloat16)
    scores = (
        jnp.einsum("qd,ld->ql", query_rows, key_line, preferred_element_type=jnp.float32)
        * score_scale
    )
    scores = scores + shift_line.astype(jnp.float32)[None, :]
    log_keep = jax.nn.log_sigmoid(-scores)
    inside = lax.cumsum(log_keep, axis=1, reverse=True) - log_keep
    weights = jnp.exp(jax.nn.log_sigmoid(scores) + inside).astype(jnp.bfloat16)
    read_sum = jnp.dot(weights, value_line, preferred_element_type=jnp.float32)
    first_out = row_norm(read_sum, out_gain).astype(jnp.bfloat16)
    return (
        key_line.reshape(1, 1, length, head_size),
        value_line.reshape(1, 1, length, head_size),
        shift_line.reshape(1, 1, length),
        first_out[None],
    )

CORES = 2
PASS_LAST = 64


def rms(entries):
    return lax.rsqrt(jnp.mean(entries * entries, axis=-1, keepdims=True) + epsilon)


def fused(
    nx,
    nz,
    x_ref,
    gain_ref,
    kw_ref,
    vw_ref,
    key_gain_ref,
    shift_ref,
    query_ref,
    query_gain_ref,
    out_gain_ref,
    key_out,
    value_out,
    shift_out,
    read_out,
    x_buf,
    n_buf,
    w_buf,
    k_send,
    v_send,
    k_line,
    v_line,
    shift_buf,
    local_sem,
    out_sem,
    act_sem,
    shift_sem,
    za_sem,
    ya_sem,
    xa_sem,
    yb_sem,
    xb_sem,
    zb_sem,
    kv_sem,
):
    sp, tp = lax.axis_index("sp"), lax.axis_index("tp")
    z, x = sp // nx, sp % nx
    y, core = tp // CORES, tp % CORES
    rows = x_ref.shape[1]
    depth, head = kw_ref.shape
    width = gain_ref.shape[1]
    cut = depth - PASS_LAST
    far_y = 1 - y

    def device(zz, xx, yy, cc):
        return (zz * nx + xx, yy * CORES + cc)

    def zs(d):
        return lax.rem(z + d, nz)

    partner = device(z, x, y, 1 - core)
    y_peer = device(z, x, far_y, core)
    x_peer = device(z, 1 - x, y, core)
    z_peers = [device(zs(d), x, y, core) for d in range(1, nz)]
    cross = device(z, x, far_y, 1 - core)

    own = pl.multiple_of(sp * depth, depth)
    locals_ = [
        pltpu.make_async_copy(
            kw_ref, w_buf.at[y, pl.ds(own, depth), pl.ds(0, head)], local_sem.at[0]
        ),
        pltpu.make_async_copy(
            vw_ref, w_buf.at[y, pl.ds(own, depth), pl.ds(head, head)], local_sem.at[1]
        ),
        pltpu.make_async_copy(
            x_ref.at[0], x_buf.at[core], local_sem.at[2]
        ),
    ]
    for c in locals_:
        c.start()

    barrier = pltpu.get_barrier_semaphore()
    greeted = [partner, y_peer, x_peer, cross] + z_peers
    for peer in greeted:
        pl.semaphore_signal(
            barrier, inc=1, device_id=peer, device_id_type=pl.DeviceIdType.MESH
        )
    pl.semaphore_wait(barrier, len(greeted))

    started = []

    def send(src, dst, sems, index, peer):
        c = pltpu.make_async_remote_copy(
            src_ref=src,
            dst_ref=dst,
            send_sem=sems.at[0, index],
            recv_sem=sems.at[1, index],
            device_id=peer,
            device_id_type=pl.DeviceIdType.MESH,
        )
        c.start()
        started.append(c)
        return c

    def arrived(dst, sems, index, peer):
        pltpu.make_async_remote_copy(
            src_ref=dst,
            dst_ref=dst,
            send_sem=sems.at[0, index],
            recv_sem=sems.at[1, index],
            device_id=peer,
            device_id_type=pl.DeviceIdType.MESH,
        ).wait_recv()

    def part_a(zz, xx, yy):
        at = pl.multiple_of((zz * nx + xx) * depth, depth)
        return w_buf.at[yy, pl.ds(at, cut), :]

    def part_b(zz, xx, yy):
        at = pl.multiple_of((zz * nx + xx) * depth + cut, PASS_LAST)
        return w_buf.at[yy, pl.ds(at, PASS_LAST), :]

    def send_part(part, sems, index, peer):
        send(part, part, sems, index, peer)

    locals_[0].wait()
    locals_[1].wait()
    b_own, a_own = part_b(z, x, y), part_a(z, x, y)
    send_part(b_own, yb_sem, 0, y_peer)
    send_part(b_own, xb_sem, 0, x_peer)
    send_part(a_own, ya_sem, 0, y_peer)
    send_part(a_own, xa_sem, 0, x_peer)
    for d in range(1, nz):
        send_part(a_own, za_sem, d - 1, z_peers[d - 1])
    for d in range(1, nz):
        send_part(b_own, zb_sem, d - 1, z_peers[d - 1])
    act = send(x_ref.at[0], x_buf.at[core], act_sem, 0, partner)
    for i, peer in enumerate((partner, y_peer, cross)):
        send(shift_ref.at[0], shift_buf.at[tp], shift_sem, i, peer)

    def normalise(which):
        tile = 16

        def body(i, _):
            at = pl.multiple_of(i * tile, tile)
            v = x_buf[which, pl.ds(at, tile), :].astype(jnp.float32)
            n_buf[which, pl.ds(at, tile), :] = (v * rms(v) * gain_ref[...]).astype(jnp.bfloat16)
            return 0

        lax.fori_loop(0, rows // tile, body, 0, unroll=2)

    locals_[2].wait()
    normalise(core)

    arrived(part_b(z, x, far_y), yb_sem, 0, y_peer)
    send_part(part_b(z, x, far_y), xb_sem, 1, x_peer)
    for d in range(1, nz):
        send_part(part_b(z, x, far_y), zb_sem, (nz - 1) + d - 1, z_peers[d - 1])
    arrived(part_b(z, 1 - x, y), xb_sem, 0, x_peer)
    for d in range(1, nz):
        send_part(part_b(z, 1 - x, y), zb_sem, 2 * (nz - 1) + d - 1, z_peers[d - 1])
    arrived(part_a(z, x, far_y), ya_sem, 0, y_peer)
    send_part(part_a(z, x, far_y), xa_sem, nz, x_peer)
    for d in range(1, nz):
        arrived(part_a(zs(nz - d), x, y), za_sem, d - 1, z_peers[nz - d - 1])
        send_part(part_a(zs(nz - d), x, y), ya_sem, d, y_peer)
        if d == 1:
            send_part(part_a(zs(nz - d), x, y), xa_sem, d, x_peer)
    arrived(part_b(z, 1 - x, far_y), xb_sem, 1, x_peer)
    for d in range(1, nz):
        send_part(part_b(z, 1 - x, far_y), zb_sem, 3 * (nz - 1) + d - 1, z_peers[d - 1])
    for d in range(1, nz):
        arrived(part_a(zs(nz - d), x, far_y), ya_sem, d, y_peer)
        send_part(part_a(zs(nz - d), x, far_y), xa_sem, nz + d, x_peer)
    for d in range(2, nz):
        send_part(part_a(zs(nz - d), x, y), xa_sem, d, x_peer)

    arrived(x_buf.at[1 - core], act_sem, 0, partner)
    normalise(1 - core)

    def project(which, yy):
        raw = jnp.dot(n_buf[which], w_buf[yy], preferred_element_type=jnp.float32)
        keys = raw[:, :head]
        keys = keys * rms(keys) * key_gain_ref[...]
        return keys.astype(jnp.bfloat16), raw[:, head:].astype(jnp.bfloat16)

    for d in range(nz):
        arrived(part_a(zs(nz - d) if d else z, 1 - x, far_y), xa_sem, nz + d, x_peer)
    for g, (xx, yy) in ((1, (x, far_y)), (3, (1 - x, far_y))):
        for d in range(1, nz):
            arrived(
                part_b(zs(nz - d), xx, yy), zb_sem, g * (nz - 1) + d - 1, z_peers[nz - d - 1]
            )
    base = y * CORES * rows
    far_base = far_y * CORES * rows
    for c in range(CORES):
        keys, values = project(c, far_y)
        k_send[c], v_send[c] = keys, values
        at = pl.multiple_of(base + c * rows, rows)
        send(k_send.at[c], k_line.at[pl.ds(at, rows), :], kv_sem, 2 * c, y_peer)
        send(v_send.at[c], v_line.at[pl.ds(at, rows), :], kv_sem, 2 * c + 1, y_peer)

    arrived(part_a(z, 1 - x, y), xa_sem, 0, x_peer)
    for d in range(1, nz):
        arrived(part_a(zs(nz - d), 1 - x, y), xa_sem, d, x_peer)
    for g, (xx, yy) in ((0, (x, y)), (2, (1 - x, y))):
        for d in range(1, nz):
            arrived(
                part_b(zs(nz - d), xx, yy), zb_sem, g * (nz - 1) + d - 1, z_peers[nz - d - 1]
            )
    for c in range(CORES):
        keys, values = project(c, y)
        at = pl.multiple_of(base + c * rows, rows)
        k_line[pl.ds(at, rows), :] = keys
        v_line[pl.ds(at, rows), :] = values

    shift_buf[tp] = shift_ref[0]
    arrived(shift_buf.at[y * CORES + 1 - core], shift_sem, 0, partner)
    arrived(shift_buf.at[far_y * CORES + core], shift_sem, 1, y_peer)
    arrived(shift_buf.at[far_y * CORES + 1 - core], shift_sem, 2, cross)
    tps = shift_buf.shape[0]
    pieces = []
    for t in range(tps):
        block = shift_buf[t].astype(jnp.float32)
        mine = lax.broadcasted_iota(jnp.int32, block.shape, 0) == tp
        pieces.append(jnp.sum(jnp.where(mine, block, 0.0), axis=0, keepdims=True))
    shifts = jnp.concatenate(pieces, axis=1)
    shift_out[0] = shifts.astype(jnp.bfloat16)

    for c in range(CORES):
        at = pl.multiple_of(far_base + c * rows, rows)
        arrived(k_line.at[pl.ds(at, rows), :], kv_sem, 2 * c, y_peer)
        arrived(v_line.at[pl.ds(at, rows), :], kv_sem, 2 * c + 1, y_peer)
    outs = [
        pltpu.make_async_copy(k_line, key_out.at[0, 0], out_sem.at[0]),
        pltpu.make_async_copy(v_line, value_out.at[0, 0], out_sem.at[1]),
    ]
    for c in outs:
        c.start()

    heads = query_ref.shape[1]
    q = query_ref[0].astype(jnp.float32)
    q = q * rms(q) * query_gain_ref[...]
    q = jnp.concatenate([q, q], axis=0).astype(jnp.bfloat16)
    scores = lax.dot_general(
        q, k_line[...], (((1,), (1,)), ((), ())), preferred_element_type=jnp.float32
    )
    scores = scores * (1.0 / head**0.5) + shifts
    soft = jnp.log1p(jnp.exp(-jnp.abs(scores)))
    log_keep = -(jnp.maximum(scores, 0.0) + soft)
    log_stop = jnp.minimum(scores, 0.0) - soft
    lanes = 128
    count = scores.shape[1] // lanes
    later = (
        lax.broadcasted_iota(jnp.int32, (lanes, lanes), 0)
        > lax.broadcasted_iota(jnp.int32, (lanes, lanes), 1)
    ).astype(jnp.float32)
    blocks = [log_keep[:, i * lanes : (i + 1) * lanes] for i in range(count)]
    within = jnp.dot(
        jnp.concatenate(blocks, axis=0),
        later,
        precision=lax.Precision.HIGHEST,
        preferred_element_type=jnp.float32,
    )
    m = q.shape[0]
    carry = jnp.zeros((m, 1), jnp.float32)
    inside = [None] * count
    for i in range(count - 1, -1, -1):
        inside[i] = within[i * m : (i + 1) * m] + carry
        carry = carry + jnp.sum(blocks[i], axis=1, keepdims=True)
    weights = jnp.exp(log_stop + jnp.concatenate(inside, axis=1)).astype(jnp.bfloat16)
    read = jnp.dot(weights, v_line[...], preferred_element_type=jnp.float32)[:heads]
    read_out[0] = (read * rms(read) * out_gain_ref[...]).astype(jnp.bfloat16)

    for c in outs:
        c.wait()
    for c in started:
        c.wait_send()


def lanes_of_cores(nx, nz, *args):
    (x, gain, kw, vw, key_gain, shift, query, query_gain, out_gain) = args
    tp = lax.axis_size("tp")
    rows, width = x.shape[1:]
    depth, head = kw.shape
    sp = nx * nz
    length = rows * tp
    vmem = pl.BlockSpec(memory_space=pltpu.VMEM)
    hbm = pl.BlockSpec(memory_space=pl.ANY)
    bf16 = jnp.bfloat16
    dma = lambda n: pltpu.SemaphoreType.DMA((2, n))
    return pl.pallas_call(
        functools.partial(fused, nx, nz),
        out_shape=(
            jax.ShapeDtypeStruct((1, 1, length, head), bf16),
            jax.ShapeDtypeStruct((1, 1, length, head), bf16),
            jax.ShapeDtypeStruct((1, 1, length), bf16),
            jax.ShapeDtypeStruct(query.shape, bf16),
        ),
        in_specs=[hbm, vmem, hbm, hbm] + [vmem] * 5,
        out_specs=(hbm, hbm, vmem, vmem),
        scratch_shapes=[
            pltpu.VMEM((CORES, rows, width), bf16),
            pltpu.VMEM((CORES, rows, width), bf16),
            pltpu.VMEM((tp // CORES, sp * depth, 2 * head), bf16),
            pltpu.VMEM((CORES, rows, head), bf16),
            pltpu.VMEM((CORES, rows, head), bf16),
            pltpu.VMEM((length, head), bf16),
            pltpu.VMEM((length, head), bf16),
            pltpu.VMEM((tp,) + shift.shape[1:], bf16),
            pltpu.SemaphoreType.DMA((3,)),
            pltpu.SemaphoreType.DMA((2,)),
            dma(1),
            dma(3),
            dma(nz - 1),
            dma(nz),
            dma(2 * nz),
            dma(1),
            dma(2),
            dma(4 * (nz - 1)),
            dma(2 * CORES),
        ],
        compiler_params=pltpu.CompilerParams(
            collective_id=0, has_side_effects=True, vmem_limit_bytes=48 * 1024 * 1024
        ),
        name="fused",
    )(
        x,
        gain.reshape(1, width),
        kw,
        vw,
        key_gain.reshape(1, head),
        shift,
        query,
        query_gain.reshape(1, head),
        out_gain.reshape(1, head),
    )


def x_extent(mesh):
    spots = [getattr(d, "coords", None) for d in mesh.devices.flat]
    if any(s is None for s in spots):
        return 2
    return len({s[0] for s in spots})


def solution(mesh):
    nx = x_extent(mesh)
    nz = mesh.shape["sp"] // nx
    small = nx == 2 and mesh.shape["tp"] == KVH and nz > 1 and nx * nz == mesh.shape["sp"]
    body = functools.partial(lanes_of_cores, nx, nz) if small else shards
    placed = (
        P("sp", "tp", None),
        P(),
        P("sp", "tp"),
        P("sp", "tp"),
        P(),
        P("sp", None, "tp"),
        P("sp", "tp", None),
        P(),
        P(),
    )
    return jax.shard_map(
        body,
        mesh=mesh,
        in_specs=placed,
        out_specs=(
            P("sp", "tp", None, None),
            P("sp", "tp", None, None),
            P("sp", "tp", None),
            P("sp", "tp", None),
        ),
        check_vma=False,
    )
```

```python
import functools

import jax
import jax.numpy as jnp
from jax import lax
from jax.experimental import pallas as pl
from jax.experimental.pallas import tpu as pltpu
from jax.sharding import PartitionSpec as P

KVH = 4


epsilon = 1e-06


def row_norm(value_entries, scaling):
    return (
        value_entries
        * lax.rsqrt(jnp.mean(value_entries * value_entries, axis=-1, keepdims=True) + epsilon)
        * scaling
    )


def shards(
    layer_input,
    input_gain,
    key_weight,
    value_weight,
    key_gain,
    stop_shift,
    new_query,
    query_gain,
    out_gain,
):
    groups = lax.axis_size("tp")
    copies = groups // KVH
    row_count = layer_input.shape[1]
    head_size = new_query.shape[2]
    score_scale = 1.0 / head_size**0.5
    normed = row_norm(layer_input[0].astype(jnp.float32), input_gain).astype(jnp.bfloat16)
    stacked = jnp.stack((key_weight, value_weight), 0)
    full_depth = lax.all_gather(stacked, "sp", axis=1, tiled=True)
    projected = jnp.einsum(
        "rd,kdc->krc",
        normed,
        lax.all_gather(full_depth, "tp", axis=2, tiled=True),
        preferred_element_type=jnp.float32,
    )
    key_rows = row_norm(projected[0].reshape(row_count, KVH, head_size), key_gain).astype(
        jnp.bfloat16
    )
    value_rows = projected[1].reshape(row_count, KVH, head_size).astype(jnp.bfloat16)
    local_shift = stop_shift[0]
    key_slots = jnp.repeat(key_rows, copies, axis=1)
    value_slots = jnp.repeat(value_rows, copies, axis=1)
    shift_slots = jnp.repeat(local_shift.T, copies, axis=1)
    key_got, value_got, shift_got = (
        lax.all_to_all(key_slots, "tp", split_axis=1, concat_axis=0, tiled=True),
        lax.all_to_all(value_slots, "tp", split_axis=1, concat_axis=0, tiled=True),
        lax.all_to_all(shift_slots, "tp", split_axis=1, concat_axis=0, tiled=True),
    )
    key_line = key_got[:, 0, :]
    value_line = value_got[:, 0, :]
    shift_line = shift_got[:, 0]
    length = key_line.shape[0]
    query_rows = row_norm(new_query[0].astype(jnp.float32), query_gain).astype(jnp.bfloat16)
    scores = (
        jnp.einsum("qd,ld->ql", query_rows, key_line, preferred_element_type=jnp.float32)
        * score_scale
    )
    scores = scores + shift_line.astype(jnp.float32)[None, :]
    log_keep = jax.nn.log_sigmoid(-scores)
    inside = lax.cumsum(log_keep, axis=1, reverse=True) - log_keep
    weights = jnp.exp(jax.nn.log_sigmoid(scores) + inside).astype(jnp.bfloat16)
    read_sum = jnp.dot(weights, value_line, preferred_element_type=jnp.float32)
    first_out = row_norm(read_sum, out_gain).astype(jnp.bfloat16)
    return (
        key_line.reshape(1, 1, length, head_size),
        value_line.reshape(1, 1, length, head_size),
        shift_line.reshape(1, 1, length),
        first_out[None],
    )

CORES = 2
VMEM_LIMIT = 67043328


def rms(entries):
    return lax.rsqrt(jnp.mean(entries * entries, axis=-1, keepdims=True) + epsilon)


def gather_kernel(
    nx,
    nz,
    x_ref,
    gain_ref,
    kw_ref,
    vw_ref,
    key_gain_ref,
    shift_ref,
    k_line,
    v_line,
    shift_buf,
    x_buf,
    n_buf,
    k_buf,
    v_buf,
    k_send,
    v_send,
    gain_buf,
    key_gain_buf,
    local_sem,
    act_sem,
    shift_sem,
    zk_sem,
    yk_sem,
    xk_sem,
    yv_sem,
    zv_sem,
    xv_sem,
    kv_sem,
):
    sp, tp = lax.axis_index("sp"), lax.axis_index("tp")
    z, x = sp // nx, sp % nx
    y, core = tp // CORES, tp % CORES
    rows = x_ref.shape[1]
    depth = kw_ref.shape[0]
    far_y = 1 - y

    def device(zz, xx, yy, cc):
        return (zz * nx + xx, yy * CORES + cc)

    def zs(d):
        return lax.rem(z + d, nz)

    def zb(d):
        return lax.rem(z + nz - d, nz) if d else z

    partner = device(z, x, y, 1 - core)
    y_peer = device(z, x, far_y, core)
    x_peer = device(z, 1 - x, y, core)
    z_peers = [device(zs(d), x, y, core) for d in range(1, nz)]
    cross = device(z, x, far_y, 1 - core)

    own = pl.multiple_of(sp * depth, depth)
    locals_ = [
        pltpu.make_async_copy(kw_ref, k_buf.at[y, pl.ds(own, depth), :], local_sem.at[0]),
        pltpu.make_async_copy(vw_ref, v_buf.at[y, pl.ds(own, depth), :], local_sem.at[1]),
        pltpu.make_async_copy(x_ref.at[0], x_buf.at[core], local_sem.at[2]),
        pltpu.make_async_copy(gain_ref, gain_buf, local_sem.at[3]),
        pltpu.make_async_copy(key_gain_ref, key_gain_buf, local_sem.at[4]),
        pltpu.make_async_copy(shift_ref.at[0], shift_buf.at[tp], local_sem.at[5]),
    ]
    for c in locals_:
        c.start()

    barrier = pltpu.get_barrier_semaphore()
    greeted = [partner, y_peer, x_peer, cross] + z_peers
    for peer in greeted:
        pl.semaphore_signal(
            barrier, inc=1, device_id=peer, device_id_type=pl.DeviceIdType.MESH
        )
    pl.semaphore_wait(barrier, len(greeted))

    started = []

    def remote(src, dst, sems, index, peer):
        return pltpu.make_async_remote_copy(
            src_ref=src,
            dst_ref=dst,
            send_sem=sems.at[0, index],
            recv_sem=sems.at[1, index],
            device_id=peer,
            device_id_type=pl.DeviceIdType.MESH,
        )

    def send(src, dst, sems, index, peer):
        c = remote(src, dst, sems, index, peer)
        c.start()
        started.append(c)

    def arrived(dst, sems, index, peer):
        remote(dst, dst, sems, index, peer).wait_recv()

    def part(buf, zz, xx, yy):
        at = pl.multiple_of((zz * nx + xx) * depth, depth)
        return buf.at[yy, pl.ds(at, depth), :]

    def pass_on(block, sems, index, peer):
        send(block, block, sems, index, peer)

    locals_[0].wait()
    k_own = part(k_buf, z, x, y)
    pass_on(k_own, yk_sem, 0, y_peer)
    pass_on(k_own, xk_sem, 0, x_peer)
    for d in range(1, nz):
        pass_on(k_own, zk_sem, d - 1, z_peers[d - 1])
    locals_[1].wait()
    v_own = part(v_buf, z, x, y)
    pass_on(v_own, yv_sem, 0, y_peer)
    pass_on(v_own, xv_sem, 0, x_peer)
    send(x_ref.at[0], x_buf.at[core], act_sem, 0, partner)
    for i, peer in enumerate((partner, y_peer, cross)):
        send(shift_ref.at[0], shift_buf.at[tp], shift_sem, i, peer)

    tile = 16

    def normalise(which, first, last):
        def body(i, _):
            at = pl.multiple_of(i * tile, tile)
            v = x_buf[which, pl.ds(at, tile), :].astype(jnp.float32)
            n_buf[which, pl.ds(at, tile), :] = (v * rms(v) * gain_buf[...]).astype(jnp.bfloat16)
            return 0

        lax.fori_loop(first, last, body, 0, unroll=2)

    for c in locals_[2:]:
        c.wait()
    tiles = rows // tile
    normalise(core, 0, tiles)

    arrived(part(k_buf, z, x, far_y), yk_sem, 0, y_peer)
    pass_on(part(k_buf, z, x, far_y), xk_sem, nz, x_peer)
    arrived(part(v_buf, z, x, far_y), yv_sem, 0, y_peer)
    for d in range(1, nz):
        pass_on(part(v_buf, z, x, far_y), zv_sem, nz - 1 + d - 1, z_peers[d - 1])
    for d in range(1, nz):
        pass_on(v_own, zv_sem, d - 1, z_peers[d - 1])
    for d in range(1, nz):
        block = part(k_buf, zb(d), x, y)
        arrived(block, zk_sem, d - 1, z_peers[nz - d - 1])
        pass_on(block, yk_sem, d, y_peer)
        if d == 1:
            pass_on(part(v_buf, z, x, far_y), xv_sem, nz, x_peer)
            pass_on(block, xk_sem, d, x_peer)
            arrived(x_buf.at[1 - core], act_sem, 0, partner)
        first = (d - 1) * tiles // (nz - 1) // 2 * 2
        last = tiles if d == nz - 1 else d * tiles // (nz - 1) // 2 * 2
        normalise(1 - core, first, last)
    for d in range(1, nz):
        block = part(k_buf, zb(d), x, far_y)
        arrived(block, yk_sem, d, y_peer)
        pass_on(block, xk_sem, nz + d, x_peer)
    for d in range(1, nz):
        block = part(v_buf, zb(d), x, far_y)
        arrived(block, zv_sem, nz - 1 + d - 1, z_peers[nz - d - 1])
        pass_on(block, xv_sem, nz + d, x_peer)
    for d in range(2, nz):
        pass_on(part(k_buf, zb(d), x, y), xk_sem, d, x_peer)

    def keys_of(which, yy):
        keys = jnp.dot(n_buf[which], k_buf[yy], preferred_element_type=jnp.float32)
        return (keys * rms(keys) * key_gain_buf[...]).astype(jnp.bfloat16)

    def values_of(which, yy):
        return jnp.dot(n_buf[which], v_buf[yy], preferred_element_type=jnp.float32).astype(
            jnp.bfloat16
        )

    def span(yy, c):
        return pl.ds(pl.multiple_of((yy * CORES + c) * rows, rows), rows)

    for d in range(nz):
        arrived(part(k_buf, zb(d), 1 - x, far_y), xk_sem, nz + d, x_peer)
    for c in range(CORES):
        k_send[c] = keys_of(c, far_y)
        send(k_send.at[c], k_line.at[span(y, c), :], kv_sem, c, y_peer)
    for d in range(nz):
        arrived(part(v_buf, zb(d), 1 - x, far_y), xv_sem, nz + d, x_peer)
    for c in range(CORES):
        v_send[c] = values_of(c, far_y)
        send(v_send.at[c], v_line.at[span(y, c), :], kv_sem, CORES + c, y_peer)
    for d in range(1, nz):
        block = part(v_buf, zb(d), x, y)
        arrived(block, zv_sem, d - 1, z_peers[nz - d - 1])
        pass_on(block, xv_sem, d, x_peer)

    for d in range(nz):
        arrived(part(k_buf, zb(d), 1 - x, y), xk_sem, d, x_peer)
    for c in range(CORES):
        k_line[span(y, c), :] = keys_of(c, y)
    for d in range(nz):
        arrived(part(v_buf, zb(d), 1 - x, y), xv_sem, d, x_peer)
    for c in range(CORES):
        v_line[span(y, c), :] = values_of(c, y)

    arrived(shift_buf.at[y * CORES + 1 - core], shift_sem, 0, partner)
    arrived(shift_buf.at[far_y * CORES + core], shift_sem, 1, y_peer)
    arrived(shift_buf.at[far_y * CORES + 1 - core], shift_sem, 2, cross)
    for c in range(CORES):
        arrived(k_line.at[span(far_y, c), :], kv_sem, c, y_peer)
        arrived(v_line.at[span(far_y, c), :], kv_sem, CORES + c, y_peer)
    for c in started:
        c.wait_send()


def read_kernel(
    k_line,
    v_line,
    shift_buf,
    query_ref,
    query_gain_ref,
    out_gain_ref,
    key_out,
    value_out,
    shift_out,
    read_out,
    query_buf,
    query_gain_buf,
    out_gain_buf,
    shift_line,
    read_line,
    in_sem,
    out_sem,
):
    ins = [
        pltpu.make_async_copy(query_ref, query_buf, in_sem.at[0]),
        pltpu.make_async_copy(query_gain_ref, query_gain_buf, in_sem.at[1]),
        pltpu.make_async_copy(out_gain_ref, out_gain_buf, in_sem.at[2]),
    ]
    outs = [
        pltpu.make_async_copy(k_line, key_out.at[0, 0], out_sem.at[0]),
        pltpu.make_async_copy(v_line, value_out.at[0, 0], out_sem.at[1]),
        pltpu.make_async_copy(shift_line, shift_out, out_sem.at[2]),
        pltpu.make_async_copy(read_line, read_out, out_sem.at[3]),
    ]
    for c in ins:
        c.start()
    outs[0].start()
    outs[1].start()
    tp = lax.axis_index("tp")
    head = k_line.shape[1]
    pieces = []
    for t in range(shift_buf.shape[0]):
        block = shift_buf[t].astype(jnp.float32)
        mine = lax.broadcasted_iota(jnp.int32, block.shape, 0) == tp
        pieces.append(jnp.sum(jnp.where(mine, block, 0.0), axis=0, keepdims=True))
    shifts = jnp.concatenate(pieces, axis=1)
    shift_line[0] = shifts.astype(jnp.bfloat16)
    outs[2].start()
    for c in ins:
        c.wait()

    heads = query_buf.shape[1]
    q = query_buf[0].astype(jnp.float32)
    q = q * rms(q) * query_gain_buf[...]
    q = jnp.concatenate([q, q], axis=0).astype(jnp.bfloat16)
    scores = lax.dot_general(
        q, k_line[...], (((1,), (1,)), ((), ())), preferred_element_type=jnp.float32
    )
    scores = scores * (1.0 / head**0.5) + shifts
    soft = jnp.log1p(jnp.exp(-jnp.abs(scores)))
    log_keep = -(jnp.maximum(scores, 0.0) + soft)
    log_stop = jnp.minimum(scores, 0.0) - soft
    lanes = 128
    count = scores.shape[1] // lanes
    later = (
        lax.broadcasted_iota(jnp.int32, (lanes, lanes), 0)
        > lax.broadcasted_iota(jnp.int32, (lanes, lanes), 1)
    ).astype(jnp.float32)
    blocks = [log_keep[:, i * lanes : (i + 1) * lanes] for i in range(count)]
    within = jnp.dot(
        jnp.concatenate(blocks, axis=0),
        later,
        precision=lax.Precision.HIGHEST,
        preferred_element_type=jnp.float32,
    )
    m = q.shape[0]
    carry = jnp.zeros((m, 1), jnp.float32)
    inside = [None] * count
    for i in range(count - 1, -1, -1):
        inside[i] = within[i * m : (i + 1) * m] + carry
        carry = carry + jnp.sum(blocks[i], axis=1, keepdims=True)
    weights = jnp.exp(log_stop + jnp.concatenate(inside, axis=1)).astype(jnp.bfloat16)
    read = jnp.dot(weights, v_line[...], preferred_element_type=jnp.float32)[:heads]
    read_line[0] = (read * rms(read) * out_gain_buf[...]).astype(jnp.bfloat16)
    outs[3].start()
    for c in outs:
        c.wait()


def lanes_of_cores(nx, nz, *args):
    (x, gain, kw, vw, key_gain, shift, query, query_gain, out_gain) = args
    tp = lax.axis_size("tp")
    rows, width = x.shape[1:]
    depth, head = kw.shape
    sp = nx * nz
    length = rows * tp
    vmem = pl.BlockSpec(memory_space=pltpu.VMEM)
    hbm = pl.BlockSpec(memory_space=pltpu.HBM)
    bf16 = jnp.bfloat16
    dma = lambda n: pltpu.SemaphoreType.DMA((2, n))
    k_line, v_line, shifts = pl.pallas_call(
        functools.partial(gather_kernel, nx, nz),
        out_shape=(
            jax.ShapeDtypeStruct((length, head), bf16),
            jax.ShapeDtypeStruct((length, head), bf16),
            jax.ShapeDtypeStruct((tp,) + shift.shape[1:], bf16),
        ),
        in_specs=[hbm] * 6,
        out_specs=(vmem, vmem, vmem),
        scratch_shapes=[
            pltpu.VMEM((CORES, rows, width), bf16),
            pltpu.VMEM((CORES, rows, width), bf16),
            pltpu.VMEM((tp // CORES, sp * depth, head), bf16),
            pltpu.VMEM((tp // CORES, sp * depth, head), bf16),
            pltpu.VMEM((CORES, rows, head), bf16),
            pltpu.VMEM((CORES, rows, head), bf16),
            pltpu.VMEM((1, width), jnp.float32),
            pltpu.VMEM((1, head), jnp.float32),
            pltpu.SemaphoreType.DMA((6,)),
            dma(1),
            dma(3),
            dma(nz - 1),
            dma(nz),
            dma(2 * nz),
            dma(1),
            dma(2 * (nz - 1)),
            dma(2 * nz),
            dma(2 * CORES),
        ],
        compiler_params=pltpu.CompilerParams(
            collective_id=0, has_side_effects=True, vmem_limit_bytes=VMEM_LIMIT
        ),
        name="gather_project",
    )(x, gain.reshape(1, width), kw, vw, key_gain.reshape(1, head), shift)
    return pl.pallas_call(
        read_kernel,
        out_shape=(
            jax.ShapeDtypeStruct((1, 1, length, head), bf16),
            jax.ShapeDtypeStruct((1, 1, length, head), bf16),
            jax.ShapeDtypeStruct((1, 1, length), bf16),
            jax.ShapeDtypeStruct(query.shape, bf16),
        ),
        in_specs=[vmem] * 3 + [hbm] * 3,
        out_specs=(hbm,) * 4,
        scratch_shapes=[
            pltpu.VMEM(query.shape, bf16),
            pltpu.VMEM((1, head), jnp.float32),
            pltpu.VMEM((1, head), jnp.float32),
            pltpu.VMEM((1, 1, length), bf16),
            pltpu.VMEM(query.shape, bf16),
            pltpu.SemaphoreType.DMA((3,)),
            pltpu.SemaphoreType.DMA((4,)),
        ],
        compiler_params=pltpu.CompilerParams(vmem_limit_bytes=VMEM_LIMIT),
        name="read",
    )(k_line, v_line, shifts, query, query_gain.reshape(1, head), out_gain.reshape(1, head))


def x_extent(mesh):
    spots = [getattr(d, "coords", None) for d in mesh.devices.flat]
    if any(s is None for s in spots):
        return 2
    return len({s[0] for s in spots})


def solution(mesh):
    nx = x_extent(mesh)
    nz = mesh.shape["sp"] // nx
    small = nx == 2 and mesh.shape["tp"] == KVH and nz > 1 and nx * nz == mesh.shape["sp"]
    body = functools.partial(lanes_of_cores, nx, nz) if small else shards
    placed = (
        P("sp", "tp", None),
        P(),
        P("sp", "tp"),
        P("sp", "tp"),
        P(),
        P("sp", None, "tp"),
        P("sp", "tp", None),
        P(),
        P(),
    )
    return jax.shard_map(
        body,
        mesh=mesh,
        in_specs=placed,
        out_specs=(
            P("sp", "tp", None, None),
            P("sp", "tp", None, None),
            P("sp", "tp", None),
            P("sp", "tp", None),
        ),
        check_vma=False,
    )
```

```python
import functools

import jax
import jax.numpy as jnp
from jax import lax
from jax.experimental import pallas as pl
from jax.experimental.pallas import tpu as pltpu
from jax.sharding import PartitionSpec as P

KVH = 4


epsilon = 1e-06


def row_norm(value_entries, scaling):
    return (
        value_entries
        * lax.rsqrt(jnp.mean(value_entries * value_entries, axis=-1, keepdims=True) + epsilon)
        * scaling
    )


def shards(
    layer_input,
    input_gain,
    key_weight,
    value_weight,
    key_gain,
    stop_shift,
    new_query,
    query_gain,
    out_gain,
):
    groups = lax.axis_size("tp")
    copies = groups // KVH
    row_count = layer_input.shape[1]
    head_size = new_query.shape[2]
    score_scale = 1.0 / head_size**0.5
    normed = row_norm(layer_input[0].astype(jnp.float32), input_gain).astype(jnp.bfloat16)
    stacked = jnp.stack((key_weight, value_weight), 0)
    full_depth = lax.all_gather(stacked, "sp", axis=1, tiled=True)
    projected = jnp.einsum(
        "rd,kdc->krc",
        normed,
        lax.all_gather(full_depth, "tp", axis=2, tiled=True),
        preferred_element_type=jnp.float32,
    )
    key_rows = row_norm(projected[0].reshape(row_count, KVH, head_size), key_gain).astype(
        jnp.bfloat16
    )
    value_rows = projected[1].reshape(row_count, KVH, head_size).astype(jnp.bfloat16)
    local_shift = stop_shift[0]
    key_slots = jnp.repeat(key_rows, copies, axis=1)
    value_slots = jnp.repeat(value_rows, copies, axis=1)
    shift_slots = jnp.repeat(local_shift.T, copies, axis=1)
    key_got, value_got, shift_got = (
        lax.all_to_all(key_slots, "tp", split_axis=1, concat_axis=0, tiled=True),
        lax.all_to_all(value_slots, "tp", split_axis=1, concat_axis=0, tiled=True),
        lax.all_to_all(shift_slots, "tp", split_axis=1, concat_axis=0, tiled=True),
    )
    key_line = key_got[:, 0, :]
    value_line = value_got[:, 0, :]
    shift_line = shift_got[:, 0]
    length = key_line.shape[0]
    query_rows = row_norm(new_query[0].astype(jnp.float32), query_gain).astype(jnp.bfloat16)
    scores = (
        jnp.einsum("qd,ld->ql", query_rows, key_line, preferred_element_type=jnp.float32)
        * score_scale
    )
    scores = scores + shift_line.astype(jnp.float32)[None, :]
    log_keep = jax.nn.log_sigmoid(-scores)
    inside = lax.cumsum(log_keep, axis=1, reverse=True) - log_keep
    weights = jnp.exp(jax.nn.log_sigmoid(scores) + inside).astype(jnp.bfloat16)
    read_sum = jnp.dot(weights, value_line, preferred_element_type=jnp.float32)
    first_out = row_norm(read_sum, out_gain).astype(jnp.bfloat16)
    return (
        key_line.reshape(1, 1, length, head_size),
        value_line.reshape(1, 1, length, head_size),
        shift_line.reshape(1, 1, length),
        first_out[None],
    )

CORES = 2
Z_EIGHTHS = 2
VMEM_LIMIT = 67043328


def rms(entries):
    return lax.rsqrt(jnp.mean(entries * entries, axis=-1, keepdims=True) + epsilon)


def gather_kernel(
    nx,
    nz,
    x_ref,
    gain_ref,
    kw_ref,
    vw_ref,
    key_gain_ref,
    shift_ref,
    query_ref,
    query_gain_ref,
    k_line,
    v_line,
    shift_line,
    weight_line,
    shift_buf,
    query_buf,
    query_gain_buf,
    x_buf,
    n_buf,
    k_buf,
    v_buf,
    k_send,
    v_send,
    gain_buf,
    key_gain_buf,
    local_sem,
    act_sem,
    shift_sem,
    zk_sem,
    yk_sem,
    xk_sem,
    yv_sem,
    zv_sem,
    xv_sem,
    kv_sem,
):
    sp, tp = lax.axis_index("sp"), lax.axis_index("tp")
    z, x = sp // nx, sp % nx
    y, core = tp // CORES, tp % CORES
    rows = x_ref.shape[1]
    depth = kw_ref.shape[0]
    far_y = 1 - y

    def device(zz, xx, yy, cc):
        return (zz * nx + xx, yy * CORES + cc)

    def zs(d):
        return lax.rem(z + d, nz)

    def zb(d):
        return lax.rem(z + nz - d, nz) if d else z

    partner = device(z, x, y, 1 - core)
    y_peer = device(z, x, far_y, core)
    x_peer = device(z, 1 - x, y, core)
    z_peers = [device(zs(d), x, y, core) for d in range(1, nz)]
    cross = device(z, x, far_y, 1 - core)

    own = pl.multiple_of(sp * depth, depth)
    locals_ = [
        pltpu.make_async_copy(kw_ref, k_buf.at[y, pl.ds(own, depth), :], local_sem.at[0]),
        pltpu.make_async_copy(vw_ref, v_buf.at[y, pl.ds(own, depth), :], local_sem.at[1]),
        pltpu.make_async_copy(x_ref.at[0], x_buf.at[core], local_sem.at[2]),
        pltpu.make_async_copy(gain_ref, gain_buf, local_sem.at[3]),
        pltpu.make_async_copy(key_gain_ref, key_gain_buf, local_sem.at[4]),
        pltpu.make_async_copy(shift_ref.at[0], shift_buf.at[tp], local_sem.at[5]),
        pltpu.make_async_copy(query_ref, query_buf, local_sem.at[6]),
        pltpu.make_async_copy(query_gain_ref, query_gain_buf, local_sem.at[7]),
    ]
    for c in locals_:
        c.start()

    barrier = pltpu.get_barrier_semaphore()
    greeted = [partner, y_peer, x_peer, cross] + z_peers
    for peer in greeted:
        pl.semaphore_signal(
            barrier, inc=1, device_id=peer, device_id_type=pl.DeviceIdType.MESH
        )
    pl.semaphore_wait(barrier, len(greeted))

    started = []

    def remote(src, dst, sems, index, peer):
        return pltpu.make_async_remote_copy(
            src_ref=src,
            dst_ref=dst,
            send_sem=sems.at[0, index],
            recv_sem=sems.at[1, index],
            device_id=peer,
            device_id_type=pl.DeviceIdType.MESH,
        )

    def send(src, dst, sems, index, peer):
        c = remote(src, dst, sems, index, peer)
        c.start()
        started.append(c)

    def arrived(dst, sems, index, peer):
        remote(dst, dst, sems, index, peer).wait_recv()

    def part(buf, zz, xx, yy):
        at = pl.multiple_of((zz * nx + xx) * depth, depth)
        return buf.at[yy, pl.ds(at, depth), :]

    def half(zz, xx, yy, i):
        cut = depth * Z_EIGHTHS // 8
        first, size = ((0, depth - cut), (depth - cut, cut))[i]
        at = pl.multiple_of((zz * nx + xx) * depth + first, depth // 8)
        return v_buf.at[yy, pl.ds(at, size), :]

    def pass_on(block, sems, index, peer):
        send(block, block, sems, index, peer)

    locals_[0].wait()
    k_own = part(k_buf, z, x, y)
    pass_on(k_own, yk_sem, 0, y_peer)
    pass_on(k_own, xk_sem, 0, x_peer)
    for d in range(1, nz):
        pass_on(k_own, zk_sem, d - 1, z_peers[d - 1])
    locals_[1].wait()
    v_own = part(v_buf, z, x, y)
    pass_on(v_own, yv_sem, 0, y_peer)
    pass_on(v_own, xv_sem, 0, x_peer)
    send(x_ref.at[0], x_buf.at[core], act_sem, 0, partner)
    for i, peer in enumerate((partner, y_peer, cross)):
        send(shift_ref.at[0], shift_buf.at[tp], shift_sem, i, peer)

    tile = 16

    def normalise(which, first, last):
        def body(i, _):
            at = pl.multiple_of(i * tile, tile)
            v = x_buf[which, pl.ds(at, tile), :].astype(jnp.float32)
            n_buf[which, pl.ds(at, tile), :] = (v * rms(v) * gain_buf[...]).astype(jnp.bfloat16)
            return 0

        lax.fori_loop(first, last, body, 0, unroll=2)

    for c in locals_[2:]:
        c.wait()
    tiles = rows // tile
    normalise(core, 0, tiles)

    arrived(part(k_buf, z, 1 - x, y), xk_sem, 0, x_peer)
    pass_on(part(k_buf, z, 1 - x, y), yk_sem, nz, y_peer)
    arrived(part(v_buf, z, x, far_y), yv_sem, 0, y_peer)
    for d in range(1, nz):
        pass_on(part(v_buf, z, x, far_y), zv_sem, nz - 1 + d - 1, z_peers[d - 1])
    for d in range(1, nz):
        pass_on(v_own, zv_sem, d - 1, z_peers[d - 1])
    for d in range(1, nz):
        block = part(k_buf, zb(d), x, y)
        arrived(block, zk_sem, d - 1, z_peers[nz - d - 1])
        pass_on(block, yk_sem, d, y_peer)
        pass_on(block, xk_sem, d, x_peer)
        if d == 1:
            pass_on(part(v_buf, z, x, far_y), xv_sem, nz, x_peer)
            arrived(part(v_buf, z, 1 - x, y), xv_sem, 0, x_peer)
            for e in range(1, nz):
                pass_on(half(z, 1 - x, y, 1), zv_sem, 2 * (nz - 1) + e - 1, z_peers[e - 1])
            arrived(x_buf.at[1 - core], act_sem, 0, partner)
        first = (d - 1) * tiles // (nz - 1) // 2 * 2
        last = tiles if d == nz - 1 else d * tiles // (nz - 1) // 2 * 2
        normalise(1 - core, first, last)
    for d in range(1, nz):
        block = part(k_buf, zb(d), 1 - x, y)
        arrived(block, xk_sem, d, x_peer)
        pass_on(block, yk_sem, nz + d, y_peer)
    for d in range(1, nz):
        block = part(v_buf, zb(d), x, far_y)
        arrived(block, zv_sem, nz - 1 + d - 1, z_peers[nz - d - 1])
        pass_on(block, xv_sem, nz + d, x_peer)

    def keys_of(which, yy):
        keys = jnp.dot(n_buf[which], k_buf[yy], preferred_element_type=jnp.float32)
        return (keys * rms(keys) * key_gain_buf[...]).astype(jnp.bfloat16)

    def values_of(which, yy):
        return jnp.dot(n_buf[which], v_buf[yy], preferred_element_type=jnp.float32).astype(
            jnp.bfloat16
        )

    def span(yy, c):
        return pl.ds(pl.multiple_of((yy * CORES + c) * rows, rows), rows)

    for d in range(nz):
        arrived(part(k_buf, zb(d), x, far_y), yk_sem, d, y_peer)
        arrived(part(k_buf, zb(d), 1 - x, far_y), yk_sem, nz + d, y_peer)
    for c in range(CORES):
        k_send[c] = keys_of(c, far_y)
        send(k_send.at[c], k_line.at[span(y, c), :], kv_sem, c, y_peer)
    for d in range(1, nz):
        block = part(v_buf, zb(d), x, y)
        arrived(block, zv_sem, d - 1, z_peers[nz - d - 1])
        pass_on(half(zb(d), x, y, 0), xv_sem, d, x_peer)
    for d in range(nz):
        arrived(part(v_buf, zb(d), 1 - x, far_y), xv_sem, nz + d, x_peer)
    for c in range(CORES):
        v_send[c] = values_of(c, far_y)
        send(v_send.at[c], v_line.at[span(y, c), :], kv_sem, CORES + c, y_peer)

    for c in range(CORES):
        k_line[span(y, c), :] = keys_of(c, y)
    arrived(shift_buf.at[y * CORES + 1 - core], shift_sem, 0, partner)
    arrived(shift_buf.at[far_y * CORES + core], shift_sem, 1, y_peer)
    arrived(shift_buf.at[far_y * CORES + 1 - core], shift_sem, 2, cross)
    for c in range(CORES):
        arrived(k_line.at[span(far_y, c), :], kv_sem, c, y_peer)
    pieces = []
    for t in range(shift_buf.shape[0]):
        block = shift_buf[t].astype(jnp.float32)
        mine = lax.broadcasted_iota(jnp.int32, block.shape, 0) == tp
        pieces.append(jnp.sum(jnp.where(mine, block, 0.0), axis=0, keepdims=True))
    shifts = jnp.concatenate(pieces, axis=1)
    shift_line[0] = shifts.astype(jnp.bfloat16)
    head = k_line.shape[1]
    q = query_buf[0].astype(jnp.float32)
    q = q * rms(q) * query_gain_buf[...]
    q = jnp.concatenate([q, q], axis=0).astype(jnp.bfloat16)
    scores = lax.dot_general(
        q, k_line[...], (((1,), (1,)), ((), ())), preferred_element_type=jnp.float32
    )
    scores = scores * (1.0 / head**0.5) + shifts
    soft = jnp.log1p(jnp.exp(-jnp.abs(scores)))
    log_keep = -(jnp.maximum(scores, 0.0) + soft)
    log_stop = jnp.minimum(scores, 0.0) - soft
    lanes = 128
    count = scores.shape[1] // lanes
    later = (
        lax.broadcasted_iota(jnp.int32, (lanes, lanes), 0)
        > lax.broadcasted_iota(jnp.int32, (lanes, lanes), 1)
    ).astype(jnp.float32)
    blocks = [log_keep[:, i * lanes : (i + 1) * lanes] for i in range(count)]
    within = jnp.dot(
        jnp.concatenate(blocks, axis=0),
        later,
        precision=lax.Precision.HIGHEST,
        preferred_element_type=jnp.float32,
    )
    m = q.shape[0]
    carry = jnp.zeros((m, 1), jnp.float32)
    inside = [None] * count
    for i in range(count - 1, -1, -1):
        inside[i] = within[i * m : (i + 1) * m] + carry
        carry = carry + jnp.sum(blocks[i], axis=1, keepdims=True)
    weight_line[...] = jnp.exp(log_stop + jnp.concatenate(inside, axis=1)).astype(jnp.bfloat16)

    for d in range(1, nz):
        arrived(half(zb(d), 1 - x, y, 0), xv_sem, d, x_peer)
        arrived(
            half(zb(d), 1 - x, y, 1), zv_sem, 2 * (nz - 1) + d - 1, z_peers[nz - d - 1]
        )
    for c in range(CORES):
        v_line[span(y, c), :] = values_of(c, y)
    for c in range(CORES):
        arrived(v_line.at[span(far_y, c), :], kv_sem, CORES + c, y_peer)
    for c in started:
        c.wait_send()


def read_kernel(
    k_line,
    v_line,
    shift_line,
    weight_line,
    out_gain_ref,
    key_out,
    value_out,
    shift_out,
    read_out,
    k_buf,
    v_buf,
    s_buf,
    w_buf,
    gain_buf,
    read_line,
    in_sem,
    out_sem,
):
    pairs = [(v_line, v_buf), (weight_line, w_buf), (out_gain_ref, gain_buf)]
    pairs += [(k_line, k_buf), (shift_line, s_buf)]
    ins = [pltpu.make_async_copy(a, b, in_sem.at[i]) for i, (a, b) in enumerate(pairs)]
    outs = [
        pltpu.make_async_copy(v_buf, value_out.at[0, 0], out_sem.at[1]),
        pltpu.make_async_copy(k_buf, key_out.at[0, 0], out_sem.at[0]),
        pltpu.make_async_copy(s_buf, shift_out, out_sem.at[2]),
        pltpu.make_async_copy(read_line, read_out, out_sem.at[3]),
    ]
    for c in ins:
        c.start()
    ins[0].wait()
    outs[0].start()
    ins[3].wait()
    outs[1].start()
    ins[4].wait()
    outs[2].start()
    ins[1].wait()
    ins[2].wait()
    heads = read_line.shape[1]
    read = jnp.dot(w_buf[...], v_buf[...], preferred_element_type=jnp.float32)[:heads]
    read_line[0] = (read * rms(read) * gain_buf[...]).astype(jnp.bfloat16)
    outs[3].start()
    for c in outs:
        c.wait()


def lanes_of_cores(nx, nz, *args):
    (x, gain, kw, vw, key_gain, shift, query, query_gain, out_gain) = args
    tp = lax.axis_size("tp")
    rows, width = x.shape[1:]
    depth, head = kw.shape
    sp = nx * nz
    length = rows * tp
    vmem = pl.BlockSpec(memory_space=pltpu.VMEM)
    hbm = pl.BlockSpec(memory_space=pltpu.HBM)
    bf16 = jnp.bfloat16
    dma = lambda n: pltpu.SemaphoreType.DMA((2, n))
    lines = pl.pallas_call(
        functools.partial(gather_kernel, nx, nz),
        out_shape=(
            jax.ShapeDtypeStruct((length, head), bf16),
            jax.ShapeDtypeStruct((length, head), bf16),
            jax.ShapeDtypeStruct((1, 1, length), bf16),
            jax.ShapeDtypeStruct((2 * query.shape[1], length), bf16),
        ),
        in_specs=[hbm] * 8,
        out_specs=(vmem,) * 4,
        scratch_shapes=[
            pltpu.VMEM((tp,) + shift.shape[1:], bf16),
            pltpu.VMEM(query.shape, bf16),
            pltpu.VMEM((1, head), jnp.float32),
            pltpu.VMEM((CORES, rows, width), bf16),
            pltpu.VMEM((CORES, rows, width), bf16),
            pltpu.VMEM((tp // CORES, sp * depth, head), bf16),
            pltpu.VMEM((tp // CORES, sp * depth, head), bf16),
            pltpu.VMEM((CORES, rows, head), bf16),
            pltpu.VMEM((CORES, rows, head), bf16),
            pltpu.VMEM((1, width), jnp.float32),
            pltpu.VMEM((1, head), jnp.float32),
            pltpu.SemaphoreType.DMA((8,)),
            dma(1),
            dma(3),
            dma(nz - 1),
            dma(2 * nz),
            dma(nz),
            dma(1),
            dma(3 * (nz - 1)),
            dma(2 * nz),
            dma(2 * CORES),
        ],
        compiler_params=pltpu.CompilerParams(
            collective_id=0, has_side_effects=True, vmem_limit_bytes=VMEM_LIMIT
        ),
        name="gather_project",
    )(x, gain.reshape(1, width), kw, vw, key_gain.reshape(1, head), shift, query, query_gain.reshape(1, head))
    return pl.pallas_call(
        read_kernel,
        out_shape=(
            jax.ShapeDtypeStruct((1, 1, length, head), bf16),
            jax.ShapeDtypeStruct((1, 1, length, head), bf16),
            jax.ShapeDtypeStruct((1, 1, length), bf16),
            jax.ShapeDtypeStruct(query.shape, bf16),
        ),
        in_specs=[hbm] * 5,
        out_specs=(hbm,) * 4,
        scratch_shapes=[
            pltpu.VMEM((length, head), bf16),
            pltpu.VMEM((length, head), bf16),
            pltpu.VMEM((1, 1, length), bf16),
            pltpu.VMEM((2 * query.shape[1], length), bf16),
            pltpu.VMEM((1, head), jnp.float32),
            pltpu.VMEM(query.shape, bf16),
            pltpu.SemaphoreType.DMA((5,)),
            pltpu.SemaphoreType.DMA((4,)),
        ],
        compiler_params=pltpu.CompilerParams(vmem_limit_bytes=VMEM_LIMIT),
        name="read",
    )(*lines, out_gain.reshape(1, head))


def x_extent(mesh):
    spots = [getattr(d, "coords", None) for d in mesh.devices.flat]
    if any(s is None for s in spots):
        return 2
    return len({s[0] for s in spots})


def solution(mesh):
    nx = x_extent(mesh)
    nz = mesh.shape["sp"] // nx
    small = nx == 2 and mesh.shape["tp"] == KVH and nz > 1 and nx * nz == mesh.shape["sp"]
    body = functools.partial(lanes_of_cores, nx, nz) if small else shards
    placed = (
        P("sp", "tp", None),
        P(),
        P("sp", "tp"),
        P("sp", "tp"),
        P(),
        P("sp", None, "tp"),
        P("sp", "tp", None),
        P(),
        P(),
    )
    return jax.shard_map(
        body,
        mesh=mesh,
        in_specs=placed,
        out_specs=(
            P("sp", "tp", None, None),
            P("sp", "tp", None, None),
            P("sp", "tp", None),
            P("sp", "tp", None),
        ),
        check_vma=False,
    )
```
